32 devices in a mesh: rep: 2 (over x), fs: 8 (over z, y), tp: 2 (over core).
Axes of the slice: x: 2, y: 2, z: 4, core: 2. Of those that a mesh axis runs over, the one named last changes fastest.
Arguments:
- x_next: bfloat16 [6144, 2048], P(('rep', 'fs')), may hold values from -6 to 6
- value_next: bfloat16 [6144, 3072], P(('rep', 'fs'), 'tp'), may hold values from -6 to 6
- x_prev: bfloat16 [6144, 2048], P(('rep', 'fs')), may hold values from -6 to 6
- value_prev: bfloat16 [6144, 3072], P(('rep', 'fs'), 'tp'), may hold values from -6 to 6
- cotangent: bfloat16 [6144, 3072], P(('rep', 'fs'), 'tp'), may hold values from -6 to 6
- w_gate: bfloat16 [2048, 3072], P('fs', 'tp'), may hold values from -0.125 to 0.125
- conv_taps: float32 [3, 3072], P(None, 'tp'), may hold values from -3.5 to 3.5
- conv_bias: float32 [3072], P('tp'), may hold values from -3 to 3
- sum_w: float32 [2048, 3072], P('fs', 'tp'), may hold values from -6 to 6
- sum_taps: float32 [3, 3072], P(None, 'tp'), may hold values from -6 to 6
- sum_bias: float32 [3072], P('tp'), may hold values from -6 to 6
Outputs:
- hidden_next: bfloat16 [6144, 3072], P(('rep', 'fs'), 'tp')
- grad_input: bfloat16 [6144, 2048], P(('rep', 'fs'))
- grad_value: bfloat16 [6144, 3072], P(('rep', 'fs'), 'tp')
- new_sum_w: float32 [2048, 3072], P('fs', 'tp')
- new_sum_taps: float32 [3, 3072], P(None, 'tp')
- new_sum_bias: float32 [3072], P('tp')
The draws below stay inside these ranges and needn't reach their ends.
All inputs are finite; a program needn't handle non-finite values.
Results may differ from the reference program's by a relative error of at most 0.015.
Values may be sent and summed in bfloat16 or wider, within the bound.
A program may use at most 64 MiB of HBM per device.

```python
import jax
import jax.numpy as jnp
from jax import lax

D = 2048
F = 3072
TAPS = 3
SEQ_LEN = 128
TOKENS = 6144
N_TP = 2


def raised(entries, own_key, source, target, shards_of, factor):
    def block_of(axis_at):
        return (jnp.arange(entries.shape[axis_at]) // (entries.shape[axis_at] // shards_of)).reshape((-1,) + (1,) * (entries.ndim - 1 - axis_at))

    first = jax.random.permutation(own_key, shards_of)[block_of(target)]
    other_side = (block_of(target) + shards_of // 2) % shards_of
    return jnp.where((block_of(source) == first) | (block_of(source) == other_side), factor * entries, entries)


def shard_levels(rng, shape, shards, low, top_value):
    def one(dim, parts):
        steps = jax.random.uniform(jax.random.fold_in(jax.random.fold_in(rng, 6), dim), (parts,), jnp.float32, low / len(shards), top_value / len(shards))
        return jnp.repeat(jnp.exp(steps), shape[dim] // parts).reshape((-1,) + (1,) * (len(shape) - dim - 1))

    factor_of = one(*shards[0])
    for cut in shards[1:]:
        factor_of = factor_of * one(*cut)
    return factor_of


def noise(own_key, extent, spread, reach, pieces=(), held_as=jnp.bfloat16):
    drawn = jax.random.normal(own_key, extent, jnp.float32) * spread
    if len(pieces) > 0:
        drawn = shard_levels(own_key, extent, pieces, -0.22, 0.18) * drawn
    return jnp.clip(drawn, min=-reach, max=reach).astype(held_as)


def noise_with(key, dims, width, limit, split, heavy, kind=jnp.bfloat16):
    values = width * jax.random.normal(key, dims, jnp.float32)
    if split:
        values = values * shard_levels(key, dims, split, -0.22, 0.18)
    return jnp.clip(raised(values, jax.random.fold_in(key, 3), *heavy), -limit, limit).astype(kind)


def setup_inputs(seed: int = 0) -> dict:
    splits = jax.random.split(jax.random.key(seed), 12)
    x_next = noise(splits[0], (TOKENS, D), 1.0, 6.0, ((0, 16),))
    value_next = noise(splits[1], (TOKENS, F), 1.0, 6.0, ((0, 16), (1, 2)))
    x_prev = noise_with(splits[2], (TOKENS, D), 1.0, 6.0, ((0, 16),), (0, 1, 16, 2.0))
    value_prev = noise(splits[3], (TOKENS, F), 1.0, 6.0, ((0, 16), (1, 2)))
    cotangent = noise_with(splits[4], (TOKENS, F), 1.0, 6.0, ((0, 16), (1, 2)), (0, 1, 16, 2.0))
    w_gate = noise(splits[5], (D, F), D ** -0.5, 0.125, ((0, 8), (1, 2)))
    conv_taps = noise(splits[6], (TAPS, F), TAPS ** -0.5, 3.5, ((1, 2),), jnp.float32)
    conv_bias = noise(splits[7], (F,), 0.5, 3.0, ((0, 2),), jnp.float32)
    sum_w = noise(splits[8], (D, F), 1.0, 6.0, ((0, 8), (1, 2)), jnp.float32)
    sum_taps = noise(splits[9], (TAPS, F), 1.0, 6.0, ((1, 2),), jnp.float32)
    sum_bias = noise(splits[10], (F,), 1.0, 6.0, ((0, 2),), jnp.float32)
    return dict(x_next=x_next, value_next=value_next, x_prev=x_prev, value_prev=value_prev, cotangent=cotangent, w_gate=w_gate, conv_taps=conv_taps, conv_bias=conv_bias, sum_w=sum_w, sum_taps=sum_taps, sum_bias=sum_bias)


def lagged(values, offset, position):
    count_rows = values.shape[0]
    shifted_rows = jnp.concatenate((jnp.zeros((offset, values.shape[1]), values.dtype), values[:count_rows - offset]), axis=0)
    return jnp.where((position >= offset)[:, None], shifted_rows, jnp.zeros_like(shifted_rows))


def leading(values, offset, position):
    shifted_rows = jnp.concatenate((values[offset:], jnp.zeros((offset, values.shape[1]), values.dtype)), axis=0)
    return jnp.where((position < SEQ_LEN - offset)[:, None], shifted_rows, jnp.zeros_like(shifted_rows))


def convolve(up_rows, conv_taps, conv_bias, position):
    values = up_rows.astype(jnp.float32)
    result = jnp.zeros(values.shape, jnp.float32) + conv_bias[None, :]
    for tap_index in range(TAPS):
        result = result + conv_taps[tap_index][None, :] * lagged(values, TAPS - 1 - tap_index, position)
    return result


def reference(x_next, value_next, x_prev, value_prev, cotangent, w_gate, conv_taps, conv_bias, sum_w, sum_taps, sum_bias):
    position = jnp.arange(x_next.shape[0]) % SEQ_LEN
    up_next = jnp.dot(x_next, w_gate, preferred_element_type=jnp.float32).astype(jnp.bfloat16)
    up_prev = jnp.dot(x_prev, w_gate, preferred_element_type=jnp.float32).astype(jnp.bfloat16)
    gate_next = convolve(up_next, conv_taps, conv_bias, position)
    hidden_next = (gate_next * jax.nn.sigmoid(gate_next) * value_next.astype(jnp.float32)).astype(jnp.bfloat16)
    gate_prev = convolve(up_prev, conv_taps, conv_bias, position)
    sigmoid_gate = jax.nn.sigmoid(gate_prev)
    cot_values = cotangent.astype(jnp.float32)
    grad_value = (cot_values * gate_prev * sigmoid_gate).astype(jnp.bfloat16)
    grad_gate = cot_values * value_prev.astype(jnp.float32) * sigmoid_gate * (1.0 + gate_prev * (1.0 - sigmoid_gate))
    grad_up = jnp.zeros(grad_gate.shape, jnp.float32)
    for tap_index in range(TAPS):
        grad_up = grad_up + conv_taps[tap_index][None, :] * leading(grad_gate, TAPS - 1 - tap_index, position)
    grad_up = grad_up.astype(jnp.bfloat16)
    block_width = F // N_TP
    accumulated = jnp.zeros((x_prev.shape[0], w_gate.shape[0]), jnp.float32)
    for index_block in range(N_TP):
        block_part = jnp.dot(grad_up[:, index_block * block_width:(index_block + 1) * block_width],
                             w_gate[:, index_block * block_width:(index_block + 1) * block_width].T,
                             preferred_element_type=jnp.float32)
        accumulated = accumulated + lax.optimization_barrier(block_part.astype(jnp.bfloat16)).astype(jnp.float32)
    grad_input = accumulated.astype(jnp.bfloat16)
    grad_scale = float(x_prev.shape[0]) ** -0.5
    grad_w = jnp.dot(x_prev.T, grad_up, preferred_element_type=jnp.float32) * grad_scale
    up_values = up_prev.astype(jnp.float32)
    grad_taps = jnp.stack([jnp.sum(grad_gate * lagged(up_values, TAPS - 1 - tap_index, position), axis=0) for tap_index in range(TAPS)], axis=0) * grad_scale
    grad_bias = jnp.sum(grad_gate, axis=0) * grad_scale
    return (hidden_next, grad_input, grad_value, sum_w + grad_w, sum_taps + grad_taps, sum_bias + grad_bias)
```

```python
import functools

import jax
import jax.numpy as jnp
from jax import lax
from jax.experimental import pallas as pl
from jax.experimental.pallas import tpu as pltpu
from jax.sharding import PartitionSpec as P

SEQ_LEN = 128
MESH = pl.DeviceIdType.MESH
VMEM = pltpu.VMEM
IN_VMEM = pl.BlockSpec(memory_space=pltpu.VMEM)


def lagged(values, offset, position):
    count_rows = values.shape[0]
    shifted_rows = jnp.concatenate(
        (jnp.zeros((offset, values.shape[1]), values.dtype), values[: count_rows - offset]), axis=0
    )
    return jnp.where((position >= offset)[:, None], shifted_rows, jnp.zeros_like(shifted_rows))


def leading(values, offset, position):
    shifted_rows = jnp.concatenate(
        (values[offset:], jnp.zeros((offset, values.shape[1]), values.dtype)), axis=0
    )
    return jnp.where(
        (position < SEQ_LEN - offset)[:, None], shifted_rows, jnp.zeros_like(shifted_rows)
    )


def convolve(up_rows, conv_taps, conv_bias, position):
    values = up_rows.astype(jnp.float32)
    tap_count = conv_taps.shape[0]
    result = jnp.zeros(values.shape, jnp.float32) + conv_bias[None, :]
    for tap_index in range(tap_count):
        result = result + conv_taps[tap_index][None, :] * lagged(
            values, tap_count - 1 - tap_index, position
        )
    return result


def ring_spot(index, count):
    pair, odd = lax.div(index, 2), lax.rem(index, 2)
    return pair * (1 - odd) + (count - 1 - pair) * odd


def ring_member(spot, count):
    down = lax.div(spot, count // 2)
    return 2 * spot * (1 - down) + (2 * (count - 1 - spot) + 1) * down


def greet(devices):
    barrier = pltpu.get_barrier_semaphore()
    for device in devices:
        pl.semaphore_signal(barrier, inc=1, device_id=device, device_id_type=MESH)
    pl.semaphore_wait(barrier, len(devices))


def remote(source, target, send, recv, device):
    return pltpu.make_async_remote_copy(
        src_ref=source,
        dst_ref=target,
        send_sem=send,
        recv_sem=recv,
        device_id=device,
        device_id_type=MESH,
    )


def piece_rows(rep, quarter):
    own = pl.multiple_of(rep * (3 * quarter), quarter)
    return (pl.ds(own, quarter), pl.ds(quarter, quarter), pl.ds(2 * quarter, quarter))


def gather_kernel(count, w_ref, out_ref, ring_send, ring_recv, side_send, side_recv):
    fs, rep = lax.axis_index("fs"), lax.axis_index("rep")
    half = count // 2
    rows = piece_rows(rep, w_ref.shape[0] // 4)
    spot = ring_spot(fs, count)

    def at(offset):
        return ring_member(lax.rem(spot + offset + count, count), count)

    toward = ({"fs": at(1)}, {"fs": at(-1)})
    across = {"rep": 1 - rep}
    greet((*toward, across))

    def parts(way, step):
        return (0, 1, 2) if step < half else ((0, 1), (2,))[way]

    def hop(way, step, piece):
        owner = at((1 - step, step - 1)[way])
        block = w_ref.at[rows[piece]] if step == 1 else out_ref.at[owner, rows[piece]]
        sems = (way, step - 1, piece)
        return remote(
            block, out_ref.at[owner, rows[piece]], ring_send.at[sems], ring_recv.at[sems], toward[way]
        )

    def side(way, step):
        block = out_ref.at[at((-step, step)[way]), rows[0]]
        sems = (way, step - 1)
        return remote(block, block, side_send.at[sems], side_recv.at[sems], across)

    hops, sides = [], []
    for piece in range(3):
        for way in range(2):
            hops.append(hop(way, 1, piece))
            hops[-1].start()
    out_ref[fs] = w_ref[...]
    for step in range(1, half + 1):
        for piece in range(3):
            for way in range(2):
                if piece not in parts(way, step):
                    continue
                hop(way, step, piece).wait_recv()
                if step < half and piece in parts(way, step + 1):
                    hops.append(hop(way, step + 1, piece))
                    hops[-1].start()
                if piece == 0:
                    sides.append(side(way, step))
                    sides[-1].start()
    for copy in hops:
        copy.wait_send()
    for copy in sides:
        copy.wait()


def gather_weight(w_gate, count):
    depth, columns = w_gate.shape
    return pl.pallas_call(
        functools.partial(gather_kernel, count),
        out_shape=jax.ShapeDtypeStruct((count, depth, columns), w_gate.dtype),
        in_specs=[IN_VMEM],
        out_specs=IN_VMEM,
        scratch_shapes=[
            pltpu.SemaphoreType.DMA((2, count // 2, 3)),
            pltpu.SemaphoreType.DMA((2, count // 2, 3)),
            pltpu.SemaphoreType.DMA((2, count // 2)),
            pltpu.SemaphoreType.DMA((2, count // 2)),
        ],
        compiler_params=pltpu.CompilerParams(
            collective_id=0, has_side_effects=True, vmem_limit_bytes=40 * 2**20
        ),
        name="gather_weight",
    )(w_gate)


def reduce_kernel(
    count,
    peers,
    grad_ref,
    term_ref,
    part_ref,
    total_ref,
    terms_ref,
    parts_ref,
    side_buf,
    out_buf,
    in_buf,
    last_out,
    last_in,
    term_in,
    term_buf,
    side_send,
    side_recv,
    ring_send,
    ring_recv,
    last_send,
    last_recv,
    term_send,
    term_recv,
    pair_send,
    pair_recv,
    peer_send,
    peer_recv,
):
    fs, rep, tp = lax.axis_index("fs"), lax.axis_index("rep"), lax.axis_index("tp")
    half = count // 2
    quarter = grad_ref.shape[1] // 4
    rows, other_rows = piece_rows(rep, quarter), piece_rows(1 - rep, quarter)[0]
    spot = ring_spot(fs, count)

    def at(offset):
        return ring_member(lax.rem(spot + offset + count, count), count)

    toward = ({"fs": at(1)}, {"fs": at(-1)})
    across = {"rep": 1 - rep}
    others = [{"tp": lax.rem(tp + shift, peers)} for shift in range(1, peers)]
    greet((*toward, across, *others))

    pair = remote(term_ref, term_in, pair_send.at[0], pair_recv.at[0], across)
    pair.start()
    spread = [
        remote(part_ref, parts_ref.at[tp], peer_send.at[i], peer_recv.at[i], device)
        for i, device in enumerate(others)
    ]
    for copy in spread:
        copy.start()

    def side(offset):
        slot = offset % count
        owner = at(offset)
        return remote(
            grad_ref.at[owner, other_rows],
            side_buf.at[slot],
            side_send.at[slot],
            side_recv.at[slot],
            across,
        )

    order = [half] + [sign * k for k in range(half - 1, 0, -1) for sign in (1, -1)] + [0]
    sides = [side(offset) for offset in order]
    for copy in sides:
        copy.start()

    def parts(way, step):
        return (0, 1, 2) if step > 1 else ((0, 1), (2,))[way]

    def hop(way, step, piece):
        sems = (way, step - 1, piece)
        return remote(
            out_buf.at[sems], in_buf.at[sems], ring_send.at[sems], ring_recv.at[sems], toward[way]
        )

    def own(offset, piece):
        values = grad_ref[at(offset), rows[piece]].astype(jnp.float32)
        if piece == 0:
            values = values + side_buf[offset % count].astype(jnp.float32)
        return values

    hops = []

    def send(way, step, piece, fresh):
        offset = (half - step + 1) * (1, -1)[way]
        if piece == 0 and (way == 0 or step > 1):
            side(offset).wait_recv()
        values = own(offset, piece)
        if not fresh:
            values = values + in_buf[way, step - 2, piece].astype(jnp.float32)
        out_buf[way, step - 1, piece] = values.astype(out_buf.dtype)
        hops.append(hop(way, step, piece))
        hops[-1].start()

    def term_hop(way, step):
        block = term_buf.at[at((1 - step, step - 1)[way])]
        sems = (way, step - 1)
        return remote(block, block, term_send.at[sems], term_recv.at[sems], toward[way])

    for way, step, piece in ((0, 1, 1), (1, 1, 2), (0, 2, 2), (1, 2, 1)):
        send(way, step, piece, True)
    parts_ref[tp] = part_ref[...]
    pair.wait()
    term_buf[fs] = term_ref[...] + term_in[...]
    term_hops = [term_hop(way, 1) for way in range(2)]
    for copy in term_hops:
        copy.start()
    send(0, 1, 0, True)
    send(1, 2, 0, True)
    for step in range(1, half):
        for piece in (1, 2, 0):
            for way in range(2):
                if piece in parts(way, step):
                    hop(way, step, piece).wait_recv()
                    send(way, step + 1, piece, False)
        for way in range(2):
            term_hop(way, step).wait_recv()
            if step + 1 < half or way == 0:
                term_hops.append(term_hop(way, step + 1))
                term_hops[-1].start()
    lasts = {}
    side(0).wait_recv()
    for piece in (1, 2, 0):
        values = own(0, piece)
        for way in range(2):
            hop(way, half, piece).wait_recv()
            values = values + in_buf[way, half - 1, piece].astype(jnp.float32)
        last_out[piece] = values.astype(last_out.dtype)
        lasts[piece] = remote(
            last_out.at[piece], last_in.at[piece], last_send.at[piece], last_recv.at[piece], across
        )
        lasts[piece].start()
    term_hop(0, half).wait_recv()
    terms = term_buf[0]
    for index in range(1, count):
        terms = terms + term_buf[index]
    terms_ref[...] = terms
    for piece in (1, 2):
        lasts[piece].wait_recv()
        total_ref[rows[piece]] = last_out[piece].astype(jnp.float32) + last_in[piece].astype(
            jnp.float32
        )
    total_ref[rows[0]] = last_out[0].astype(jnp.float32)
    lasts[0].wait_recv()
    total_ref[other_rows] = last_in[0].astype(jnp.float32)
    for copy in (*sides, *hops, *term_hops, *lasts.values()):
        copy.wait_send()
    for copy in spread:
        copy.wait()


def reduce_gradients(grad_blocks, terms, part, peers):
    count, depth, columns = grad_blocks.shape
    half, quarter = count // 2, depth // 4
    dma = pltpu.SemaphoreType.DMA
    pieces = (2, half, 3)
    return pl.pallas_call(
        functools.partial(reduce_kernel, count, peers),
        out_shape=(
            jax.ShapeDtypeStruct((depth, columns), jnp.float32),
            jax.ShapeDtypeStruct(terms.shape, jnp.float32),
            jax.ShapeDtypeStruct((peers, *part.shape), part.dtype),
        ),
        in_specs=[IN_VMEM] * 3,
        out_specs=(IN_VMEM,) * 3,
        scratch_shapes=[
            VMEM((count, quarter, columns), jnp.bfloat16),
            VMEM((*pieces, quarter, columns), jnp.bfloat16),
            VMEM((*pieces, quarter, columns), jnp.bfloat16),
            VMEM((3, quarter, columns), jnp.bfloat16),
            VMEM((3, quarter, columns), jnp.bfloat16),
            VMEM(terms.shape, jnp.float32),
            VMEM((count, *terms.shape), jnp.float32),
            dma((count,)),
            dma((count,)),
            dma(pieces),
            dma(pieces),
            dma((3,)),
            dma((3,)),
            dma((2, half)),
            dma((2, half)),
            dma((1,)),
            dma((1,)),
            dma((peers,)),
            dma((peers,)),
        ],
        compiler_params=pltpu.CompilerParams(
            collective_id=1, has_side_effects=True, vmem_limit_bytes=56 * 2**20
        ),
        name="reduce_gradients",
    )(grad_blocks, terms, part)


def per_device(
    x_next,
    value_next,
    x_prev,
    value_prev,
    cotangent,
    w_gate,
    conv_taps,
    conv_bias,
    sum_w,
    sum_taps,
    sum_bias,
):
    row_count = x_next.shape[0]
    tap_count = conv_taps.shape[0]
    position = jnp.arange(row_count) % SEQ_LEN
    fs_count = lax.axis_size("fs")
    gathered = gather_weight(w_gate, fs_count).reshape(fs_count * w_gate.shape[0], w_gate.shape[1])
    up_next = jnp.dot(x_next, gathered, preferred_element_type=jnp.float32)
    up_prev = jnp.dot(x_prev, gathered, preferred_element_type=jnp.float32)
    up_next = up_next.astype(jnp.bfloat16)
    up_prev = up_prev.astype(jnp.bfloat16)
    gate_next = convolve(up_next, conv_taps, conv_bias, position)
    hidden_next = (gate_next * jax.nn.sigmoid(gate_next) * value_next.astype(jnp.float32)).astype(
        jnp.bfloat16
    )
    gate_prev = convolve(up_prev, conv_taps, conv_bias, position)
    sigmoid_gate = jax.nn.sigmoid(gate_prev)
    cot_values = cotangent.astype(jnp.float32)
    grad_value = (cot_values * gate_prev * sigmoid_gate).astype(jnp.bfloat16)
    grad_gate = (
        cot_values
        * value_prev.astype(jnp.float32)
        * sigmoid_gate
        * (1.0 + gate_prev * (1.0 - sigmoid_gate))
    )
    grad_up = jnp.zeros(grad_gate.shape, jnp.float32)
    for tap_index in range(tap_count):
        grad_up = grad_up + conv_taps[tap_index][None, :] * leading(
            grad_gate, tap_count - 1 - tap_index, position
        )
    grad_up = grad_up.astype(jnp.bfloat16)
    contract_units = (((1,), (1,)), ((), ()))
    partial_input = lax.dot_general(
        grad_up, gathered, contract_units, preferred_element_type=jnp.float32
    )
    rep_count = lax.axis_size("rep")
    grad_scale = float(row_count * rep_count * fs_count) ** (-0.5)
    up_values = up_prev.astype(jnp.float32)
    terms = jnp.stack(
        [
            jnp.sum(grad_gate * lagged(up_values, tap_count - 1 - tap_index, position), axis=0)
            for tap_index in range(tap_count)
        ]
        + [jnp.sum(grad_gate, axis=0)],
        axis=0,
    )
    grad_blocks = (
        lax.dot_general(x_prev, grad_up, (((0,), (0,)), ((), ())), preferred_element_type=jnp.float32)
        .astype(jnp.bfloat16)
        .reshape(fs_count, *w_gate.shape)
    )
    grad_rows, terms, partials = reduce_gradients(
        grad_blocks, terms, partial_input.astype(jnp.bfloat16), lax.axis_size("tp")
    )
    grad_input = jnp.sum(partials.astype(jnp.float32), axis=0).astype(jnp.bfloat16)
    return (
        hidden_next,
        grad_input,
        grad_value,
        sum_w + grad_scale * grad_rows,
        sum_taps + grad_scale * terms[:tap_count],
        sum_bias + grad_scale * terms[tap_count],
    )


def solution(mesh):
    in_specs = (
        P(("rep", "fs"), None),
        P(("rep", "fs"), "tp"),
        P(("rep", "fs"), None),
        P(("rep", "fs"), "tp"),
        P(("rep", "fs"), "tp"),
        P("fs", "tp"),
        P(None, "tp"),
        P("tp"),
        P("fs", "tp"),
        P(None, "tp"),
        P("tp"),
    )
    out_specs = (
        P(("rep", "fs"), "tp"),
        P(("rep", "fs"), None),
        P(("rep", "fs"), "tp"),
        P("fs", "tp"),
        P(None, "tp"),
        P("tp"),
    )
    return jax.shard_map(
        per_device, mesh=mesh, in_specs=in_specs, out_specs=out_specs, check_vma=False
    )
```

```python
import functools

import jax
import jax.numpy as jnp
from jax import lax
from jax.experimental import pallas as pl
from jax.experimental.pallas import tpu as pltpu
from jax.sharding import PartitionSpec as P

SEQ_LEN = 128
MESH = pl.DeviceIdType.MESH
VMEM = pltpu.VMEM
IN_VMEM = pl.BlockSpec(memory_space=pltpu.VMEM)


def lagged(values, offset, position):
    count_rows = values.shape[0]
    shifted_rows = jnp.concatenate(
        (jnp.zeros((offset, values.shape[1]), values.dtype), values[: count_rows - offset]), axis=0
    )
    return jnp.where((position >= offset)[:, None], shifted_rows, jnp.zeros_like(shifted_rows))


def leading(values, offset, position):
    shifted_rows = jnp.concatenate(
        (values[offset:], jnp.zeros((offset, values.shape[1]), values.dtype)), axis=0
    )
    return jnp.where(
        (position < SEQ_LEN - offset)[:, None], shifted_rows, jnp.zeros_like(shifted_rows)
    )


def convolve(up_rows, conv_taps, conv_bias, position):
    values = up_rows.astype(jnp.float32)
    tap_count = conv_taps.shape[0]
    result = jnp.zeros(values.shape, jnp.float32) + conv_bias[None, :]
    for tap_index in range(tap_count):
        result = result + conv_taps[tap_index][None, :] * lagged(
            values, tap_count - 1 - tap_index, position
        )
    return result


def ring_spot(index, count):
    pair, odd = lax.div(index, 2), lax.rem(index, 2)
    return pair * (1 - odd) + (count - 1 - pair) * odd


def ring_member(spot, count):
    down = lax.div(spot, count // 2)
    return 2 * spot * (1 - down) + (2 * (count - 1 - spot) + 1) * down


def greet(devices):
    barrier = pltpu.get_barrier_semaphore()
    for device in devices:
        pl.semaphore_signal(barrier, inc=1, device_id=device, device_id_type=MESH)
    pl.semaphore_wait(barrier, len(devices))


def remote(source, target, send, recv, device):
    return pltpu.make_async_remote_copy(
        src_ref=source,
        dst_ref=target,
        send_sem=send,
        recv_sem=recv,
        device_id=device,
        device_id_type=MESH,
    )


def piece_rows(rep, depth, alone):
    shared = (depth - 2 * alone) // 2
    own = pl.multiple_of(rep * (depth - alone), 16)
    return (pl.ds(own, alone), pl.ds(alone, shared), pl.ds(alone + shared, shared))


def column_tile(columns):
    return 512 if columns % 512 == 0 else columns


def gather_kernel(
    count,
    w_ref,
    x_next_ref,
    x_prev_ref,
    out_ref,
    up_next_ref,
    up_prev_ref,
    sums,
    ring_send,
    ring_recv,
    side_send,
    side_recv,
):
    fs, rep = lax.axis_index("fs"), lax.axis_index("rep")
    half = count // 2
    depth, columns = w_ref.shape
    rows = piece_rows(rep, depth, max(1, 5 * depth // 256) * 16)
    streamed, tile = depth % 128 == 0, column_tile(columns)
    spot = ring_spot(fs, count)

    def at(offset):
        return ring_member(lax.rem(spot + offset + count, count), count)

    toward = ({"fs": at(1)}, {"fs": at(-1)})
    across = {"rep": 1 - rep}
    greet((*toward, across))

    def parts(way, step):
        return (0, 1, 2) if step < half else ((0,), (1, 2))[way]

    def accumulate(offset):
        owner = at(offset)
        lanes = pl.ds(pl.multiple_of(owner * depth, 128), depth)

        @pl.loop(0, columns // tile)
        def _(index):
            where = pl.ds(pl.multiple_of(index * tile, 128), tile)
            block = out_ref[owner, :, where]
            for branch, x_ref in enumerate((x_next_ref, x_prev_ref)):
                product = jnp.dot(x_ref[:, lanes], block, preferred_element_type=jnp.float32)
                if offset != 0:
                    product = product + sums[branch, :, where]
                sums[branch, :, where] = product

    def hop(way, step, piece):
        owner = at((1 - step, step - 1)[way])
        block = w_ref.at[rows[piece]] if step == 1 else out_ref.at[owner, rows[piece]]
        sems = (way, step - 1, piece)
        return remote(
            block, out_ref.at[owner, rows[piece]], ring_send.at[sems], ring_recv.at[sems], toward[way]
        )

    def side(way, step):
        block = out_ref.at[at((-step, step)[way]), rows[0]]
        sems = (way, step - 1)
        return remote(block, block, side_send.at[sems], side_recv.at[sems], across)

    hops, sides = [], []
    for piece in range(3):
        for way in range(2):
            hops.append(hop(way, 1, piece))
            hops[-1].start()
    out_ref[fs] = w_ref[...]
    for step in range(1, half + 1):
        for piece in range(3):
            for way in range(2):
                if piece not in parts(way, step):
                    continue
                hop(way, step, piece).wait_recv()
                if step < half and piece in parts(way, step + 1):
                    hops.append(hop(way, step + 1, piece))
                    hops[-1].start()
                if piece == 0:
                    sides.append(side(way, step))
                    sides[-1].start()
        if streamed and step == 1:
            accumulate(0)
        elif streamed:
            for way in range(2):
                side(way, step - 1).wait_recv()
                accumulate((1 - step, step - 1)[way])
    side(0, half).wait_recv()
    if streamed:
        accumulate(half)
        up_next_ref[...] = sums[0].astype(up_next_ref.dtype)
        up_prev_ref[...] = sums[1].astype(up_prev_ref.dtype)
    else:
        for step in range(1, half):
            for way in range(2):
                side(way, step).wait_recv()
        whole = out_ref[...].reshape(count * depth, columns)
        for x_ref, up_ref in ((x_next_ref, up_next_ref), (x_prev_ref, up_prev_ref)):
            up = jnp.dot(x_ref[...], whole, preferred_element_type=jnp.float32)
            up_ref[...] = up.astype(up_ref.dtype)
    for copy in (*hops, *sides):
        copy.wait_send()


def gather_weight(w_gate, x_next, x_prev, count):
    depth, columns = w_gate.shape
    up = jax.ShapeDtypeStruct((x_next.shape[0], columns), jnp.bfloat16)
    return pl.pallas_call(
        functools.partial(gather_kernel, count),
        out_shape=(jax.ShapeDtypeStruct((count, depth, columns), w_gate.dtype), up, up),
        in_specs=[IN_VMEM] * 3,
        out_specs=(IN_VMEM,) * 3,
        scratch_shapes=[
            VMEM((2, *up.shape), jnp.float32),
            pltpu.SemaphoreType.DMA((2, count // 2, 3)),
            pltpu.SemaphoreType.DMA((2, count // 2, 3)),
            pltpu.SemaphoreType.DMA((2, count // 2)),
            pltpu.SemaphoreType.DMA((2, count // 2)),
        ],
        compiler_params=pltpu.CompilerParams(
            collective_id=0, has_side_effects=True, vmem_limit_bytes=40 * 2**20
        ),
        name="gather_weight",
    )(w_gate, x_next, x_prev)


def reduce_kernel(
    count,
    peers,
    x_ref,
    up_ref,
    w_ref,
    term_ref,
    total_ref,
    terms_ref,
    parts_ref,
    grad_ref,
    part_ref,
    side_buf,
    out_buf,
    in_buf,
    last_out,
    last_in,
    term_in,
    term_buf,
    side_send,
    side_recv,
    ring_send,
    ring_recv,
    last_send,
    last_recv,
    term_send,
    term_recv,
    pair_send,
    pair_recv,
    peer_send,
    peer_recv,
):
    fs, rep, tp = lax.axis_index("fs"), lax.axis_index("rep"), lax.axis_index("tp")
    half = count // 2
    depth, columns = grad_ref.shape[1:]
    tile = column_tile(columns)
    rows = piece_rows(rep, depth, depth // 4)
    other_rows = piece_rows(1 - rep, depth, depth // 4)[0]
    spot = ring_spot(fs, count)

    def at(offset):
        return ring_member(lax.rem(spot + offset + count, count), count)

    toward = ({"fs": at(1)}, {"fs": at(-1)})
    across = {"rep": 1 - rep}
    others = [{"tp": lax.rem(tp + shift, peers)} for shift in range(1, peers)]
    greet((*toward, across, *others))

    pair = remote(term_ref, term_in, pair_send.at[0], pair_recv.at[0], across)
    pair.start()
    spread = [
        remote(part_ref, parts_ref.at[tp], peer_send.at[i], peer_recv.at[i], device)
        for i, device in enumerate(others)
    ]

    def side(offset):
        slot = offset % count
        owner = at(offset)
        return remote(
            grad_ref.at[owner, other_rows],
            side_buf.at[slot],
            side_send.at[slot],
            side_recv.at[slot],
            across,
        )

    order = [half] + [sign * k for k in range(half - 1, 0, -1) for sign in (1, -1)] + [0]
    sides = []

    def multiply(offset):
        owner = at(offset)

        @pl.loop(0, columns // tile)
        def _(index):
            where = pl.ds(pl.multiple_of(index * tile, 128), tile)
            grad_ref[owner, :, where] = jnp.dot(
                x_ref[owner], up_ref[:, where], preferred_element_type=jnp.float32
            ).astype(grad_ref.dtype)

        sides.append(side(offset))
        sides[-1].start()

    joined = max(1, 128 // depth)

    def input_part(group):
        block = w_ref[group * joined : (group + 1) * joined].reshape(joined * depth, columns)
        product = lax.dot_general(
            up_ref[...], block, (((1,), (1,)), ((), ())), preferred_element_type=jnp.float32
        )
        first = group * joined * depth
        part_ref[:, first : first + joined * depth] = product.astype(part_ref.dtype)

    def parts(way, step):
        return (0, 1, 2) if step > 1 else ((0, 1), (2,))[way]

    def hop(way, step, piece):
        sems = (way, step - 1, piece)
        return remote(
            out_buf.at[sems], in_buf.at[sems], ring_send.at[sems], ring_recv.at[sems], toward[way]
        )

    def own(offset, piece):
        values = grad_ref[at(offset), rows[piece]].astype(jnp.float32)
        if piece == 0:
            values = values + side_buf[offset % count].astype(jnp.float32)
        return values

    hops = []

    def send(way, step, piece, fresh):
        offset = (half - step + 1) * (1, -1)[way]
        if piece == 0 and (way == 0 or step > 1):
            side(offset).wait_recv()
        values = own(offset, piece)
        if not fresh:
            values = values + in_buf[way, step - 2, piece].astype(jnp.float32)
        out_buf[way, step - 1, piece] = values.astype(out_buf.dtype)
        hops.append(hop(way, step, piece))
        hops[-1].start()

    def term_hop(way, step):
        block = term_buf.at[at((1 - step, step - 1)[way])]
        sems = (way, step - 1)
        return remote(block, block, term_send.at[sems], term_recv.at[sems], toward[way])

    multiply(order[0])
    send(0, 1, 1, True)
    send(1, 1, 2, True)
    multiply(order[1])
    send(0, 2, 2, True)
    multiply(order[2])
    send(1, 2, 1, True)
    for offset in order[3:]:
        multiply(offset)
    pair.wait()
    term_buf[fs] = term_ref[...] + term_in[...]
    term_hops = [term_hop(way, 1) for way in range(2)]
    for copy in term_hops:
        copy.start()
    send(0, 1, 0, True)
    send(1, 2, 0, True)
    for step in range(1, half):
        for piece in (1, 2, 0):
            for way in range(2):
                if piece in parts(way, step):
                    hop(way, step, piece).wait_recv()
                    send(way, step + 1, piece, False)
        for way in range(2):
            term_hop(way, step).wait_recv()
            if step + 1 < half or way == 0:
                term_hops.append(term_hop(way, step + 1))
                term_hops[-1].start()
        groups = count // joined
        for group in range((step - 1) * groups // (half - 1), step * groups // (half - 1)):
            input_part(group)
    for copy in spread:
        copy.start()
    parts_ref[tp] = part_ref[...]
    lasts = {}
    side(0).wait_recv()
    for piece in (1, 2, 0):
        values = own(0, piece)
        for way in range(2):
            hop(way, half, piece).wait_recv()
            values = values + in_buf[way, half - 1, piece].astype(jnp.float32)
        last_out[piece] = values.astype(last_out.dtype)
        lasts[piece] = remote(
            last_out.at[piece], last_in.at[piece], last_send.at[piece], last_recv.at[piece], across
        )
        lasts[piece].start()
    term_hop(0, half).wait_recv()
    terms = term_buf[0]
    for index in range(1, count):
        terms = terms + term_buf[index]
    terms_ref[...] = terms
    for piece in (1, 2):
        lasts[piece].wait_recv()
        total_ref[rows[piece]] = last_out[piece].astype(jnp.float32) + last_in[piece].astype(
            jnp.float32
        )
    total_ref[rows[0]] = last_out[0].astype(jnp.float32)
    lasts[0].wait_recv()
    total_ref[other_rows] = last_in[0].astype(jnp.float32)
    for copy in (*sides, *hops, *term_hops, *lasts.values()):
        copy.wait_send()
    for copy in spread:
        copy.wait()


def reduce_gradients(x_blocks, grad_up, gathered, terms, peers):
    count, depth, columns = gathered.shape
    part = jax.ShapeDtypeStruct((grad_up.shape[0], count * depth), jnp.bfloat16)
    half, quarter = count // 2, depth // 4
    dma = pltpu.SemaphoreType.DMA
    pieces = (2, half, 3)
    return pl.pallas_call(
        functools.partial(reduce_kernel, count, peers),
        out_shape=(
            jax.ShapeDtypeStruct((depth, columns), jnp.float32),
            jax.ShapeDtypeStruct(terms.shape, jnp.float32),
            jax.ShapeDtypeStruct((peers, *part.shape), part.dtype),
        ),
        in_specs=[IN_VMEM] * 4,
        out_specs=(IN_VMEM,) * 3,
        scratch_shapes=[
            VMEM(gathered.shape, jnp.bfloat16),
            VMEM(part.shape, part.dtype),
            VMEM((count, quarter, columns), jnp.bfloat16),
            VMEM((*pieces, quarter, columns), jnp.bfloat16),
            VMEM((*pieces, quarter, columns), jnp.bfloat16),
            VMEM((3, quarter, columns), jnp.bfloat16),
            VMEM((3, quarter, columns), jnp.bfloat16),
            VMEM(terms.shape, jnp.float32),
            VMEM((count, *terms.shape), jnp.float32),
            dma((count,)),
            dma((count,)),
            dma(pieces),
            dma(pieces),
            dma((3,)),
            dma((3,)),
            dma((2, half)),
            dma((2, half)),
            dma((1,)),
            dma((1,)),
            dma((peers,)),
            dma((peers,)),
        ],
        compiler_params=pltpu.CompilerParams(
            collective_id=1, has_side_effects=True, vmem_limit_bytes=56 * 2**20
        ),
        name="reduce_gradients",
    )(x_blocks, grad_up, gathered, terms)


def per_device(
    x_next,
    value_next,
    x_prev,
    value_prev,
    cotangent,
    w_gate,
    conv_taps,
    conv_bias,
    sum_w,
    sum_taps,
    sum_bias,
):
    row_count = x_next.shape[0]
    tap_count = conv_taps.shape[0]
    position = jnp.arange(row_count) % SEQ_LEN
    fs_count = lax.axis_size("fs")
    gathered, up_next, up_prev = gather_weight(w_gate, x_next, x_prev, fs_count)
    gate_next = convolve(up_next, conv_taps, conv_bias, position)
    hidden_next = (gate_next * jax.nn.sigmoid(gate_next) * value_next.astype(jnp.float32)).astype(
        jnp.bfloat16
    )
    gate_prev = convolve(up_prev, conv_taps, conv_bias, position)
    sigmoid_gate = jax.nn.sigmoid(gate_prev)
    cot_values = cotangent.astype(jnp.float32)
    grad_value = (cot_values * gate_prev * sigmoid_gate).astype(jnp.bfloat16)
    grad_gate = (
        cot_values
        * value_prev.astype(jnp.float32)
        * sigmoid_gate
        * (1.0 + gate_prev * (1.0 - sigmoid_gate))
    )
    grad_up = jnp.zeros(grad_gate.shape, jnp.float32)
    for tap_index in range(tap_count):
        grad_up = grad_up + conv_taps[tap_index][None, :] * leading(
            grad_gate, tap_count - 1 - tap_index, position
        )
    grad_up = grad_up.astype(jnp.bfloat16)
    rep_count = lax.axis_size("rep")
    grad_scale = float(row_count * rep_count * fs_count) ** (-0.5)
    up_values = up_prev.astype(jnp.float32)
    terms = jnp.stack(
        [
            jnp.sum(grad_gate * lagged(up_values, tap_count - 1 - tap_index, position), axis=0)
            for tap_index in range(tap_count)
        ]
        + [jnp.sum(grad_gate, axis=0)],
        axis=0,
    )
    peers = lax.axis_size("tp")
    x_blocks = x_prev.T.reshape(fs_count, w_gate.shape[0], row_count)
    grad_rows, terms, partials = reduce_gradients(x_blocks, grad_up, gathered, terms, peers)
    grad_input = partials[0].astype(jnp.float32)
    for peer in range(1, peers):
        grad_input = grad_input + partials[peer].astype(jnp.float32)
    grad_input = grad_input.astype(jnp.bfloat16)
    return (
        hidden_next,
        grad_input,
        grad_value,
        sum_w + grad_scale * grad_rows,
        sum_taps + grad_scale * terms[:tap_count],
        sum_bias + grad_scale * terms[tap_count],
    )


def solution(mesh):
    in_specs = (
        P(("rep", "fs"), None),
        P(("rep", "fs"), "tp"),
        P(("rep", "fs"), None),
        P(("rep", "fs"), "tp"),
        P(("rep", "fs"), "tp"),
        P("fs", "tp"),
        P(None, "tp"),
        P("tp"),
        P("fs", "tp"),
        P(None, "tp"),
        P("tp"),
    )
    out_specs = (
        P(("rep", "fs"), "tp"),
        P(("rep", "fs"), None),
        P(("rep", "fs"), "tp"),
        P("fs", "tp"),
        P(None, "tp"),
        P("tp"),
    )
    return jax.shard_map(
        per_device, mesh=mesh, in_specs=in_specs, out_specs=out_specs, check_vma=False
    )
```

```python
import functools

import jax
import jax.numpy as jnp
from jax import lax
from jax.experimental import pallas as pl
from jax.experimental.pallas import tpu as pltpu
from jax.sharding import PartitionSpec as P

SEQ_LEN = 128
MESH = pl.DeviceIdType.MESH
VMEM = pltpu.VMEM
IN_VMEM = pl.BlockSpec(memory_space=pltpu.VMEM)


def gates_kernel(
    up_next_ref,
    value_next_ref,
    up_prev_ref,
    value_prev_ref,
    cotangent_ref,
    taps_ref,
    bias_ref,
    hidden_ref,
    grad_value_ref,
    grad_up_ref,
    terms_ref,
):
    tap_count = taps_ref.shape[0]
    row_count, tile = up_next_ref.shape
    position = lax.broadcasted_iota(jnp.int32, (SEQ_LEN, tile), 0)
    lags = [tap_count - 1 - tap for tap in range(tap_count)]
    taps = [taps_ref[tap : tap + 1, :] for tap in range(tap_count)]
    bias = bias_ref[...]

    def lagged(values, offset):
        if offset == 0:
            return values
        return jnp.where(position >= offset, pltpu.roll(values, offset, 0), 0.0)

    def leading(values, offset):
        if offset == 0:
            return values
        shifted = pltpu.roll(values, SEQ_LEN - offset, 0)
        return jnp.where(position < SEQ_LEN - offset, shifted, 0.0)

    def mixed(pieces, start):
        for tap, piece in zip(taps, pieces):
            start = start + tap * piece
        return start

    sums = [jnp.zeros((1, tile), jnp.float32) for _ in range(tap_count + 1)]
    for first in range(0, row_count, SEQ_LEN):
        rows = slice(first, first + SEQ_LEN)
        up = up_next_ref[rows, :].astype(jnp.float32)
        gate = mixed([lagged(up, lag) for lag in lags], bias)
        hidden = gate * jax.nn.sigmoid(gate) * value_next_ref[rows, :].astype(jnp.float32)
        hidden_ref[rows, :] = hidden.astype(hidden_ref.dtype)
        up = up_prev_ref[rows, :].astype(jnp.float32)
        lagged_up = [lagged(up, lag) for lag in lags]
        gate = mixed(lagged_up, bias)
        sigmoid = jax.nn.sigmoid(gate)
        cot = cotangent_ref[rows, :].astype(jnp.float32)
        grad_value_ref[rows, :] = (cot * gate * sigmoid).astype(grad_value_ref.dtype)
        value = value_prev_ref[rows, :].astype(jnp.float32)
        grad_gate = cot * value * sigmoid * (1.0 + gate * (1.0 - sigmoid))
        grad_up = mixed([leading(grad_gate, lag) for lag in lags], 0.0)
        grad_up_ref[rows, :] = grad_up.astype(grad_up_ref.dtype)
        products = [grad_gate * piece for piece in lagged_up] + [grad_gate]
        sums = [
            total + jnp.sum(product, axis=0, keepdims=True)
            for total, product in zip(sums, products)
        ]
    for index, total in enumerate(sums):
        terms_ref[index : index + 1, :] = total


def gates(up_next, value_next, up_prev, value_prev, cotangent, conv_taps, conv_bias):
    row_count, columns = up_next.shape
    tap_count = conv_taps.shape[0]
    tile = 256 if columns % 256 == 0 else 128
    tall = pl.BlockSpec((row_count, tile), lambda index: (0, index))

    def flat(height):
        return pl.BlockSpec((height, tile), lambda index: (0, index))

    large = jax.ShapeDtypeStruct((row_count, columns), jnp.bfloat16)
    return pl.pallas_call(
        gates_kernel,
        grid=(columns // tile,),
        out_shape=(
            large,
            large,
            large,
            jax.ShapeDtypeStruct((tap_count + 1, columns), jnp.float32),
        ),
        in_specs=[tall] * 5 + [flat(tap_count), flat(1)],
        out_specs=(tall, tall, tall, flat(tap_count + 1)),
        name="gates",
    )(up_next, value_next, up_prev, value_prev, cotangent, conv_taps, conv_bias[None, :])


def ring_spot(index, count):
    pair, odd = lax.div(index, 2), lax.rem(index, 2)
    return pair * (1 - odd) + (count - 1 - pair) * odd


def ring_member(spot, count):
    down = lax.div(spot, count // 2)
    return 2 * spot * (1 - down) + (2 * (count - 1 - spot) + 1) * down


def greet(devices):
    barrier = pltpu.get_barrier_semaphore()
    for device in devices:
        pl.semaphore_signal(barrier, inc=1, device_id=device, device_id_type=MESH)
    pl.semaphore_wait(barrier, len(devices))


def remote(source, target, send, recv, device):
    return pltpu.make_async_remote_copy(
        src_ref=source,
        dst_ref=target,
        send_sem=send,
        recv_sem=recv,
        device_id=device,
        device_id_type=MESH,
    )


def piece_rows(rep, depth, alone):
    shared = (depth - 2 * alone) // 2
    own = pl.multiple_of(rep * (depth - alone), 16)
    return (pl.ds(own, alone), pl.ds(alone, shared), pl.ds(alone + shared, shared))


def column_tile(columns):
    return 512 if columns % 512 == 0 else columns


def gather_kernel(
    count,
    w_ref,
    x_next_ref,
    x_prev_ref,
    out_ref,
    up_next_ref,
    up_prev_ref,
    sums,
    ring_send,
    ring_recv,
    side_send,
    side_recv,
):
    fs, rep = lax.axis_index("fs"), lax.axis_index("rep")
    half = count // 2
    depth, columns = w_ref.shape
    rows = piece_rows(rep, depth, max(1, 5 * depth // 256) * 16)
    streamed, tile = depth % 128 == 0, column_tile(columns)
    spot = ring_spot(fs, count)

    def at(offset):
        return ring_member(lax.rem(spot + offset + count, count), count)

    toward = ({"fs": at(1)}, {"fs": at(-1)})
    across = {"rep": 1 - rep}
    greet((*toward, across))

    def parts(way, step):
        return (0, 1, 2) if step < half else ((0,), (1, 2))[way]

    def accumulate(offset):
        owner = at(offset)
        lanes = pl.ds(pl.multiple_of(owner * depth, 128), depth)

        @pl.loop(0, columns // tile)
        def _(index):
            where = pl.ds(pl.multiple_of(index * tile, 128), tile)
            block = out_ref[owner, :, where]
            for branch, x_ref in enumerate((x_next_ref, x_prev_ref)):
                product = jnp.dot(x_ref[:, lanes], block, preferred_element_type=jnp.float32)
                if offset != 0:
                    product = product + sums[branch, :, where]
                sums[branch, :, where] = product

    def hop(way, step, piece):
        owner = at((1 - step, step - 1)[way])
        block = w_ref.at[rows[piece]] if step == 1 else out_ref.at[owner, rows[piece]]
        sems = (way, step - 1, piece)
        return remote(
            block, out_ref.at[owner, rows[piece]], ring_send.at[sems], ring_recv.at[sems], toward[way]
        )

    def side(way, step):
        block = out_ref.at[at((-step, step)[way]), rows[0]]
        sems = (way, step - 1)
        return remote(block, block, side_send.at[sems], side_recv.at[sems], across)

    hops, sides = [], []
    for piece in range(3):
        for way in range(2):
            hops.append(hop(way, 1, piece))
            hops[-1].start()
    out_ref[fs] = w_ref[...]
    for step in range(1, half + 1):
        for piece in range(3):
            for way in range(2):
                if piece not in parts(way, step):
                    continue
                hop(way, step, piece).wait_recv()
                if step < half and piece in parts(way, step + 1):
                    hops.append(hop(way, step + 1, piece))
                    hops[-1].start()
                if piece == 0:
                    sides.append(side(way, step))
                    sides[-1].start()
        if streamed and step == 1:
            accumulate(0)
        elif streamed:
            for way in range(2):
                side(way, step - 1).wait_recv()
                accumulate((1 - step, step - 1)[way])
    side(0, half).wait_recv()
    if streamed:
        accumulate(half)
        up_next_ref[...] = sums[0].astype(up_next_ref.dtype)
        up_prev_ref[...] = sums[1].astype(up_prev_ref.dtype)
    else:
        for step in range(1, half):
            for way in range(2):
                side(way, step).wait_recv()
        whole = out_ref[...].reshape(count * depth, columns)
        for x_ref, up_ref in ((x_next_ref, up_next_ref), (x_prev_ref, up_prev_ref)):
            up = jnp.dot(x_ref[...], whole, preferred_element_type=jnp.float32)
            up_ref[...] = up.astype(up_ref.dtype)
    for copy in (*hops, *sides):
        copy.wait_send()


def gather_weight(w_gate, x_next, x_prev, count):
    depth, columns = w_gate.shape
    up = jax.ShapeDtypeStruct((x_next.shape[0], columns), jnp.bfloat16)
    return pl.pallas_call(
        functools.partial(gather_kernel, count),
        out_shape=(jax.ShapeDtypeStruct((count, depth, columns), w_gate.dtype), up, up),
        in_specs=[IN_VMEM] * 3,
        out_specs=(IN_VMEM,) * 3,
        scratch_shapes=[
            VMEM((2, *up.shape), jnp.float32),
            pltpu.SemaphoreType.DMA((2, count // 2, 3)),
            pltpu.SemaphoreType.DMA((2, count // 2, 3)),
            pltpu.SemaphoreType.DMA((2, count // 2)),
            pltpu.SemaphoreType.DMA((2, count // 2)),
        ],
        compiler_params=pltpu.CompilerParams(
            collective_id=0, has_side_effects=True, vmem_limit_bytes=40 * 2**20
        ),
        name="gather_weight",
    )(w_gate, x_next, x_prev)


def reduce_kernel(
    count,
    peers,
    x_ref,
    up_ref,
    w_ref,
    term_ref,
    total_ref,
    terms_ref,
    parts_ref,
    grad_ref,
    part_ref,
    side_buf,
    out_buf,
    in_buf,
    last_out,
    last_in,
    term_in,
    term_buf,
    side_send,
    side_recv,
    ring_send,
    ring_recv,
    last_send,
    last_recv,
    term_send,
    term_recv,
    pair_send,
    pair_recv,
    peer_send,
    peer_recv,
):
    fs, rep, tp = lax.axis_index("fs"), lax.axis_index("rep"), lax.axis_index("tp")
    half = count // 2
    depth, columns = grad_ref.shape[1:]
    tile = column_tile(columns)
    rows = piece_rows(rep, depth, depth // 4)
    other_rows = piece_rows(1 - rep, depth, depth // 4)[0]
    spot = ring_spot(fs, count)

    def at(offset):
        return ring_member(lax.rem(spot + offset + count, count), count)

    toward = ({"fs": at(1)}, {"fs": at(-1)})
    across = {"rep": 1 - rep}
    others = [{"tp": lax.rem(tp + shift, peers)} for shift in range(1, peers)]
    greet((*toward, across, *others))

    pair = remote(term_ref, term_in, pair_send.at[0], pair_recv.at[0], across)
    pair.start()
    spread = [
        remote(part_ref, parts_ref.at[tp], peer_send.at[i], peer_recv.at[i], device)
        for i, device in enumerate(others)
    ]

    def side(offset):
        slot = offset % count
        owner = at(offset)
        return remote(
            grad_ref.at[owner, other_rows],
            side_buf.at[slot],
            side_send.at[slot],
            side_recv.at[slot],
            across,
        )

    order = [half] + [sign * k for k in range(half - 1, 0, -1) for sign in (1, -1)] + [0]
    sides = []

    def multiply(offset):
        owner = at(offset)

        @pl.loop(0, columns // tile)
        def _(index):
            where = pl.ds(pl.multiple_of(index * tile, 128), tile)
            grad_ref[owner, :, where] = jnp.dot(
                x_ref[owner], up_ref[:, where], preferred_element_type=jnp.float32
            ).astype(grad_ref.dtype)

        sides.append(side(offset))
        sides[-1].start()

    joined = max(1, 128 // depth)

    def input_part(group):
        block = w_ref[group * joined : (group + 1) * joined].reshape(joined * depth, columns)
        product = lax.dot_general(
            up_ref[...], block, (((1,), (1,)), ((), ())), preferred_element_type=jnp.float32
        )
        first = group * joined * depth
        part_ref[:, first : first + joined * depth] = product.astype(part_ref.dtype)

    def parts(way, step):
        return (0, 1, 2) if step > 1 else ((0, 1), (2,))[way]

    def hop(way, step, piece):
        sems = (way, step - 1, piece)
        return remote(
            out_buf.at[sems], in_buf.at[sems], ring_send.at[sems], ring_recv.at[sems], toward[way]
        )

    def own(offset, piece):
        values = grad_ref[at(offset), rows[piece]].astype(jnp.float32)
        if piece == 0:
            values = values + side_buf[offset % count].astype(jnp.float32)
        return values

    hops = []

    def send(way, step, piece, fresh):
        offset = (half - step + 1) * (1, -1)[way]
        if piece == 0 and (way == 0 or step > 1):
            side(offset).wait_recv()
        values = own(offset, piece)
        if not fresh:
            values = values + in_buf[way, step - 2, piece].astype(jnp.float32)
        out_buf[way, step - 1, piece] = values.astype(out_buf.dtype)
        hops.append(hop(way, step, piece))
        hops[-1].start()

    def term_hop(way, step):
        block = term_buf.at[at((1 - step, step - 1)[way])]
        sems = (way, step - 1)
        return remote(block, block, term_send.at[sems], term_recv.at[sems], toward[way])

    multiply(order[0])
    send(0, 1, 1, True)
    send(1, 1, 2, True)
    multiply(order[1])
    send(0, 2, 2, True)
    multiply(order[2])
    send(1, 2, 1, True)
    for offset in order[3:]:
        multiply(offset)
    pair.wait()
    term_buf[fs] = term_ref[...] + term_in[...]
    term_hops = [term_hop(way, 1) for way in range(2)]
    for copy in term_hops:
        copy.start()
    send(0, 1, 0, True)
    send(1, 2, 0, True)
    for step in range(1, half):
        for piece in (1, 2, 0):
            for way in range(2):
                if piece in parts(way, step):
                    hop(way, step, piece).wait_recv()
                    send(way, step + 1, piece, False)
        for way in range(2):
            term_hop(way, step).wait_recv()
            if step + 1 < half or way == 0:
                term_hops.append(term_hop(way, step + 1))
                term_hops[-1].start()
        groups = count // joined
        for group in range((step - 1) * groups // (half - 1), step * groups // (half - 1)):
            input_part(group)
    for copy in spread:
        copy.start()
    parts_ref[tp] = part_ref[...]
    lasts = {}
    side(0).wait_recv()
    for piece in (1, 2, 0):
        values = own(0, piece)
        for way in range(2):
            hop(way, half, piece).wait_recv()
            values = values + in_buf[way, half - 1, piece].astype(jnp.float32)
        last_out[piece] = values.astype(last_out.dtype)
        lasts[piece] = remote(
            last_out.at[piece], last_in.at[piece], last_send.at[piece], last_recv.at[piece], across
        )
        lasts[piece].start()
    term_hop(0, half).wait_recv()
    terms = term_buf[0]
    for index in range(1, count):
        terms = terms + term_buf[index]
    terms_ref[...] = terms
    for piece in (1, 2):
        lasts[piece].wait_recv()
        total_ref[rows[piece]] = last_out[piece].astype(jnp.float32) + last_in[piece].astype(
            jnp.float32
        )
    total_ref[rows[0]] = last_out[0].astype(jnp.float32)
    lasts[0].wait_recv()
    total_ref[other_rows] = last_in[0].astype(jnp.float32)
    for copy in (*sides, *hops, *term_hops, *lasts.values()):
        copy.wait_send()
    for copy in spread:
        copy.wait()


def reduce_gradients(x_blocks, grad_up, gathered, terms, peers):
    count, depth, columns = gathered.shape
    part = jax.ShapeDtypeStruct((grad_up.shape[0], count * depth), jnp.bfloat16)
    half, quarter = count // 2, depth // 4
    dma = pltpu.SemaphoreType.DMA
    pieces = (2, half, 3)
    return pl.pallas_call(
        functools.partial(reduce_kernel, count, peers),
        out_shape=(
            jax.ShapeDtypeStruct((depth, columns), jnp.float32),
            jax.ShapeDtypeStruct(terms.shape, jnp.float32),
            jax.ShapeDtypeStruct((peers, *part.shape), part.dtype),
        ),
        in_specs=[IN_VMEM] * 4,
        out_specs=(IN_VMEM,) * 3,
        scratch_shapes=[
            VMEM(gathered.shape, jnp.bfloat16),
            VMEM(part.shape, part.dtype),
            VMEM((count, quarter, columns), jnp.bfloat16),
            VMEM((*pieces, quarter, columns), jnp.bfloat16),
            VMEM((*pieces, quarter, columns), jnp.bfloat16),
            VMEM((3, quarter, columns), jnp.bfloat16),
            VMEM((3, quarter, columns), jnp.bfloat16),
            VMEM(terms.shape, jnp.float32),
            VMEM((count, *terms.shape), jnp.float32),
            dma((count,)),
            dma((count,)),
            dma(pieces),
            dma(pieces),
            dma((3,)),
            dma((3,)),
            dma((2, half)),
            dma((2, half)),
            dma((1,)),
            dma((1,)),
            dma((peers,)),
            dma((peers,)),
        ],
        compiler_params=pltpu.CompilerParams(
            collective_id=1, has_side_effects=True, vmem_limit_bytes=56 * 2**20
        ),
        name="reduce_gradients",
    )(x_blocks, grad_up, gathered, terms)


def per_device(
    x_next,
    value_next,
    x_prev,
    value_prev,
    cotangent,
    w_gate,
    conv_taps,
    conv_bias,
    sum_w,
    sum_taps,
    sum_bias,
):
    row_count = x_next.shape[0]
    tap_count = conv_taps.shape[0]
    fs_count = lax.axis_size("fs")
    gathered, up_next, up_prev = gather_weight(w_gate, x_next, x_prev, fs_count)
    hidden_next, grad_value, grad_up, terms = gates(
        up_next, value_next, up_prev, value_prev, cotangent, conv_taps, conv_bias
    )
    rep_count = lax.axis_size("rep")
    grad_scale = float(row_count * rep_count * fs_count) ** (-0.5)
    peers = lax.axis_size("tp")
    x_blocks = x_prev.T.reshape(fs_count, w_gate.shape[0], row_count)
    grad_rows, terms, partials = reduce_gradients(x_blocks, grad_up, gathered, terms, peers)
    grad_input = partials[0].astype(jnp.float32)
    for peer in range(1, peers):
        grad_input = grad_input + partials[peer].astype(jnp.float32)
    grad_input = grad_input.astype(jnp.bfloat16)
    return (
        hidden_next,
        grad_input,
        grad_value,
        sum_w + grad_scale * grad_rows,
        sum_taps + grad_scale * terms[:tap_count],
        sum_bias + grad_scale * terms[tap_count],
    )


def solution(mesh):
    in_specs = (
        P(("rep", "fs"), None),
        P(("rep", "fs"), "tp"),
        P(("rep", "fs"), None),
        P(("rep", "fs"), "tp"),
        P(("rep", "fs"), "tp"),
        P("fs", "tp"),
        P(None, "tp"),
        P("tp"),
        P("fs", "tp"),
        P(None, "tp"),
        P("tp"),
    )
    out_specs = (
        P(("rep", "fs"), "tp"),
        P(("rep", "fs"), None),
        P(("rep", "fs"), "tp"),
        P("fs", "tp"),
        P(None, "tp"),
        P("tp"),
    )
    return jax.shard_map(
        per_device, mesh=mesh, in_specs=in_specs, out_specs=out_specs, check_vma=False
    )
```
